32 devices in a mesh: fs: 8 (over z, x), tp: 4 (over y, core).
Axes of the slice: x: 2, y: 2, z: 4, core: 2. Of those that a mesh axis runs over, the one named last changes fastest.
Arguments:
- x_late: bfloat16 [3072, 2048], P(('fs', 'tp')), may hold values from -6 to 6
- x_early: bfloat16 [3072, 2048], P(('fs', 'tp')), may hold values from -6 to 6
- cotangent: bfloat16 [3072, 2048], P(('fs', 'tp')), may hold values from -6 to 6
- up_weight: bfloat16 [2048, 4096], P('fs', 'tp'), may hold values from -0.125 to 0.125
- down_weight: bfloat16 [2048, 4096], P('fs', 'tp'), may hold values from -0.09375 to 0.09375
- up_grad_sum: float32 [2048, 4096], P('fs', 'tp'), may hold values from -24 to 24
- down_grad_sum: float32 [2048, 4096], P('fs', 'tp'), may hold values from -24 to 24
Outputs:
- output: bfloat16 [3072, 2048], P(('fs', 'tp'))
- input_grad: bfloat16 [3072, 2048], P(('fs', 'tp'))
- up_grad_new: float32 [2048, 4096], P('fs', 'tp')
- down_grad_new: float32 [2048, 4096], P('fs', 'tp')
The draws below stay inside these ranges and needn't reach their ends.
All inputs are finite; a program needn't handle non-finite values.
Results may differ from the reference program's by a relative error of at most 0.0095.
Values may be sent and summed in bfloat16 or wider, within the bound.
No kernel may reach another device: no remote copies, remote signals or barrier semaphores. Data moves between devices by JAX's collectives and lax.ppermute only.
A program may use at most 128 MiB of HBM per device.

```python
import jax
import jax.numpy as jnp
from jax import lax

D = 2048
FF = 4096
TOKENS = 3072
N_TP = 4


def raised(result, rng, source, target, shards_of, factor):
    owner, partner = [(jnp.arange(result.shape[axis_at]) // (result.shape[axis_at] // shards_of)).reshape([-1 if axis == axis_at else 1 for axis in range(result.ndim)]) for axis_at in (source, target)]
    chosen = jax.random.permutation(rng, shards_of)[partner]
    strong = (owner == chosen) | (owner == (partner + shards_of // 2) % shards_of)
    return jnp.where(strong, factor * result, result)


def block_levels(stream_key, extent, split, low, top_value):
    def one(position, shards_of):
        draws = jax.random.uniform(jax.random.fold_in(jax.random.fold_in(stream_key, 6), position), (shards_of,), jnp.float32, low / len(split), top_value / len(split))
        return jnp.repeat(jnp.exp(draws), extent[position] // shards_of).reshape((-1,) + (1,) * (len(extent) - position - 1))

    level = one(*split[0])
    for cut in split[1:]:
        level = level * one(*cut)
    return level


def normal_values(stream_key, dims, scale, limit, cuts=(), dtype=jnp.bfloat16):
    entries = jax.random.normal(stream_key, dims, jnp.float32) * scale
    if len(cuts) > 0:
        entries = block_levels(stream_key, dims, cuts, -0.22, 0.18) * entries
    return jnp.clip(entries, min=-limit, max=limit).astype(dtype)


def noise_with(own_key, extent, deviation, reach, pieces, heavy, dtype=jnp.bfloat16):
    drawn = deviation * jax.random.normal(own_key, extent, jnp.float32)
    if pieces:
        drawn = drawn * block_levels(own_key, extent, pieces, -0.22, 0.18)
    return jnp.clip(raised(drawn, jax.random.fold_in(own_key, 3), *heavy), -reach, reach).astype(dtype)


def setup_inputs(seed: int = 0) -> dict:
    arg_keys = jax.random.split(jax.random.key(seed), 8)
    x_late = normal_values(arg_keys[0], (TOKENS, D), 1.0, 6.0, ((0, 32),))
    x_early = normal_values(arg_keys[1], (TOKENS, D), 1.0, 6.0, ((0, 32),))
    cotangent = noise_with(arg_keys[2], (TOKENS, D), 0.25, 6.0, ((0, 32),), (0, 1, 32, 2.75))
    up_weight = normal_values(arg_keys[3], (D, FF), D ** -0.5, 0.125, ((0, 8), (1, 4)))
    down_weight = normal_values(arg_keys[4], (D, FF), FF ** -0.5, 0.09375, ((0, 8), (1, 4)))
    up_grad_sum = normal_values(arg_keys[5], (D, FF), 4.0, 24.0, ((0, 8), (1, 4)), jnp.float32)
    down_grad_sum = normal_values(arg_keys[6], (D, FF), 4.0, 24.0, ((0, 8), (1, 4)), jnp.float32)
    return dict(x_late=x_late, x_early=x_early, cotangent=cotangent, up_weight=up_weight, down_weight=down_weight, up_grad_sum=up_grad_sum, down_grad_sum=down_grad_sum)


def dot_last(left, right):
    return lax.dot_general(left, right, (((1,), (1,)), ((), ())), preferred_element_type=jnp.float32)


def dot_first(left, right):
    return lax.dot_general(left, right, (((0,), (0,)), ((), ())), preferred_element_type=jnp.float32)


def tp_rounded(left, right):
    stride = right.shape[1] // N_TP
    totals = jnp.zeros((left.shape[0], right.shape[0]), jnp.float32)
    for column_block in range(N_TP):
        first_col = column_block * stride
        partial_value = dot_last(left[:, first_col:first_col + stride], right[:, first_col:first_col + stride])
        rounded = lax.optimization_barrier(partial_value.astype(jnp.bfloat16))
        totals = totals + rounded.astype(jnp.float32)
    return totals.astype(jnp.bfloat16)


def reference(x_late, x_early, cotangent, up_weight, down_weight, up_grad_sum, down_grad_sum):
    pre_late = jnp.dot(x_late, up_weight, preferred_element_type=jnp.float32)
    act_late = jnp.square(jax.nn.relu(pre_late)).astype(jnp.bfloat16)
    output = tp_rounded(act_late, down_weight)
    pre_early = jnp.dot(x_early, up_weight, preferred_element_type=jnp.float32)
    act_early = jnp.square(jax.nn.relu(pre_early)).astype(jnp.bfloat16)
    grad_act = jnp.dot(cotangent, down_weight, preferred_element_type=jnp.float32)
    grad_pre = (grad_act * 2.0 * jax.nn.relu(pre_early)).astype(jnp.bfloat16)
    input_grad = tp_rounded(grad_pre, up_weight)
    up_grad_new = up_grad_sum + dot_first(x_early, grad_pre)
    down_grad_new = down_grad_sum + dot_first(cotangent, act_early)
    return (output, input_grad, up_grad_new, down_grad_new)
```

```python
import jax
import jax.numpy as jnp
from jax import lax
from jax.sharding import PartitionSpec as P


BF16, F32 = jnp.bfloat16, jnp.float32
X, Y, C = ("fs", 1), ("tp", 2), ("tp", 1)
RELAY_LIMIT = 4


def dot_plain(left, right):
    return jnp.dot(left, right, preferred_element_type=F32)


def dot_last(left, right):
    return lax.dot_general(left, right, (((1,), (1,)), ((), ())), preferred_element_type=F32)


def dot_first(left, right):
    return lax.dot_general(left, right, (((0,), (0,)), ((), ())), preferred_element_type=F32)


def solution(mesh):
    sizes = dict(mesh.shape)
    outer = sizes["fs"] // 2
    line = [[2 * z + x for z in range(outer)] for x in range(2)]

    def swap(value, hop):
        axis, mask = hop
        return lax.ppermute(value, axis, [(i, i ^ mask) for i in range(sizes[axis])])

    def shift(value, step, senders):
        pairs = [(2 * z + x, 2 * (z + step) + x) for z in senders for x in range(2)]
        return lax.ppermute(value, "fs", pairs)

    def gather_tokens(rows, first, second):
        n = rows.shape[0]
        near = swap(rows, first)
        pair = jnp.concatenate([rows, near])
        far = swap(pair, second)
        pair_c = swap(pair, C)
        far_c = swap(far, C)
        if first == X:
            parts = [pair, far, pair_c, far_c]
        else:
            parts = [rows, far[:n], near, far[n:], pair_c[:n], far_c[:n], pair_c[n:], far_c[n:]]
        return jnp.concatenate(parts)

    def scatter_tokens(part, first, second):
        n = part.shape[0] // 8
        quad = part[: 4 * n] + swap(part[4 * n :].astype(BF16), C).astype(F32)
        if first == Y:
            pair = quad[: 2 * n] + swap(quad[2 * n :].astype(BF16), Y).astype(F32)
        else:
            sent = jnp.concatenate([quad[n : 2 * n], quad[3 * n :]]).astype(BF16)
            kept = jnp.concatenate([quad[:n], quad[2 * n : 3 * n]])
            pair = kept + swap(sent, X).astype(F32)
        return (pair[:n] + swap(pair[n:].astype(BF16), second).astype(F32)).astype(BF16)

    def on_device(x_late, x_early, cotangent, up_weight, down_weight, up_grad_sum, down_grad_sum):
        place = lax.axis_index("fs")
        z, x = place // 2, place % 2
        rows, cols = up_weight.shape[0], up_weight.shape[1] // 2

        def half_swap(weight):
            mine = lax.dynamic_slice_in_dim(weight, x * cols, cols, 1)
            theirs = lax.dynamic_slice_in_dim(weight, (1 - x) * cols, cols, 1)
            return mine, swap(theirs, X)

        def spread(mine, other):
            block = jnp.where(
                x == 0, jnp.concatenate([mine, other]), jnp.concatenate([other, mine])
            )
            if outer > RELAY_LIMIT:
                return lax.all_gather(block, "fs", axis=0, tiled=True, axis_index_groups=line)
            whole = jnp.zeros(((outer + 1) * 2 * rows, cols), block.dtype)
            whole = lax.dynamic_update_slice_in_dim(whole, block, z * 2 * rows, 0)
            above, below = block, block
            for d in range(1, outer):
                above = shift(above, -1, range(1, outer - d + 1))
                below = shift(below, 1, range(d - 1, outer - 1))
                at_above = jnp.where(z + d < outer, z + d, outer)
                at_below = jnp.where(z - d >= 0, z - d, outer)
                whole = lax.dynamic_update_slice_in_dim(whole, above, at_above * 2 * rows, 0)
                whole = lax.dynamic_update_slice_in_dim(whole, below, at_below * 2 * rows, 0)
            return whole[: outer * 2 * rows]

        def collect(part):
            if outer > RELAY_LIMIT:
                return lax.psum_scatter(
                    part, "fs", scatter_dimension=0, tiled=True, axis_index_groups=line
                )

            def block(at):
                at = jnp.clip(at, 0, outer - 1)
                return lax.dynamic_slice_in_dim(part, at * 2 * rows, 2 * rows, 0)

            down, up = None, None
            for d in range(outer - 1, 0, -1):
                low, high = block(z - d), block(z + d)
                low = low if down is None else low + down.astype(F32)
                high = high if up is None else high + up.astype(F32)
                down = shift(low.astype(BF16), -1, range(d, outer))
                up = shift(high.astype(BF16), 1, range(0, outer - d))
            return block(z) + down.astype(F32) + up.astype(F32)

        def finish(total, running):
            pieces = total.reshape(2, rows, cols)
            mine = lax.dynamic_index_in_dim(pieces, x, 0, keepdims=False)
            theirs = lax.dynamic_index_in_dim(pieces, 1 - x, 0, keepdims=False)
            other = swap(theirs.astype(BF16), X).astype(F32)
            added = jnp.where(
                x == 0,
                jnp.concatenate([mine, other], axis=1),
                jnp.concatenate([other, mine], axis=1),
            )
            return running + added

        up_mine, up_other = half_swap(up_weight)
        down_mine, down_other = half_swap(down_weight)
        up_full = spread(up_mine, up_other)
        early = gather_tokens(x_early, X, Y)
        cot = gather_tokens(cotangent, Y, X)
        late = gather_tokens(x_late, X, Y)
        down_full = spread(down_mine, down_other)

        relu_early = jax.nn.relu(dot_plain(early, up_full))
        act_early = jnp.square(relu_early).astype(BF16)
        down_total = collect(dot_first(cot, act_early))
        act_late = jnp.square(jax.nn.relu(dot_plain(late, up_full))).astype(BF16)
        grad_pre = (dot_plain(cot, down_full) * 2.0 * relu_early).astype(BF16)
        up_total = collect(dot_first(early, grad_pre))
        output = scatter_tokens(dot_last(act_late, down_full), Y, X)
        input_grad = scatter_tokens(dot_last(grad_pre, up_full), X, Y)
        return (output, input_grad, finish(up_total, up_grad_sum), finish(down_total, down_grad_sum))

    token, weight = P(("fs", "tp"), None), P("fs", "tp")
    return jax.shard_map(
        on_device,
        mesh=mesh,
        in_specs=(token, token, token, weight, weight, weight, weight),
        out_specs=(token, token, weight, weight),
        check_vma=False,
    )
```
